768 devices in a mesh: fs: 96 (over z, y), tp: 8 (over x, core).
Axes of the slice: x: 4, y: 8, z: 12, core: 2. Of those that a mesh axis runs over, the one named last changes fastest.
Arguments:
- inputs: bfloat16 [49152, 2304], P('fs'), may hold values from -6 to 6
- value_cot: bfloat16 [49152, 4096], P('fs', 'tp'), may hold values from -0.026977539 to 0.026977539
- retained: bfloat16 [49152, 4096], P('fs', 'tp'), may hold values from -6 to 6
- output_cot: bfloat16 [49152, 2304], P('fs'), may hold values from -0.026977539 to 0.026977539
- proj_value: bfloat16 [2304, 192], P('fs'), may hold values from -0.125 to 0.125
- proj_output: bfloat16 [2304, 192], P('fs'), may hold values from -0.125 to 0.125
- w_value: float32 [2304, 4096], P('fs', 'tp'), may hold values from -6 to 6
- w_output: float32 [4096, 2304], P('tp', 'fs'), may hold values from -6 to 6
- first_value: float32 [192, 4096], P('fs', 'tp'), may hold values from -106 to 106
- second_value: float32 [192, 4096], P('fs', 'tp'), may hold values from 0.25 to 4
- first_output: float32 [192, 4096], P('fs', 'tp'), may hold values from -106 to 106
- second_output: float32 [192, 4096], P('fs', 'tp'), may hold values from 0.25 to 4
Outputs:
- step_value: float32 [2304, 4096], P('fs', 'tp')
- step_output: float32 [4096, 2304], P('tp', 'fs')
- copy_value: bfloat16 [2304, 4096], P(None, 'tp')
- copy_output: bfloat16 [4096, 2304], P('tp')
- new_first_value: float32 [192, 4096], P('fs', 'tp')
- new_second_value: float32 [192, 4096], P('fs', 'tp')
- new_first_output: float32 [192, 4096], P('fs', 'tp')
- new_second_output: float32 [192, 4096], P('fs', 'tp')
The draws below stay inside these ranges and needn't reach their ends.
All inputs are finite; a program needn't handle non-finite values.
Results may differ from the reference program's by a relative error of at most 0.0034.
Values may be sent and summed in bfloat16 or wider, within the bound.
No kernel may reach another device: no remote copies, remote signals or barrier semaphores. Data moves between devices by JAX's collectives and lax.ppermute only.
A program may use at most 64 MiB of HBM per device.

```python
import math
import jax
import jax.numpy as jnp
from jax import lax

D = 2304
RANK = 192
HV = 4096
TOKENS = 49152


def moment_law(key, row_total, col_total):
    row_pos = jnp.arange(row_total, dtype=jnp.float32) / row_total
    col_pos = jnp.arange(col_total, dtype=jnp.float32) / col_total
    drawn = jnp.clip(jax.random.normal(key, (row_total, col_total), jnp.float32), -6.0, 6.0)
    row_scale = 3.0 ** row_pos
    col_scale = 3.0 ** col_pos
    return drawn * row_scale[:, None] * col_scale[None, :]


def draw_first_value(key, part):
    return moment_law(jax.random.fold_in(key, 11), RANK, HV)


def draw_first_output(key, part):
    return moment_law(jax.random.fold_in(key, 23), RANK, HV)


def block_scale(own_key, dims, shards, least, largest):
    gain, own = 1.0, jax.random.fold_in(own_key, 6)
    for dim, parts in shards:
        steps = jnp.exp(jax.random.uniform(jax.random.fold_in(own, dim), (parts,), jnp.float32, least / len(shards), largest / len(shards)))
        gain = gain * jnp.repeat(steps, dims[dim] // parts).reshape([-1 if axis == dim else 1 for axis in range(len(dims))])
    return gain


def scatter_about(rng, shape, spread, most, shards=(), kind=jnp.bfloat16):
    values = jax.random.normal(rng, shape, jnp.float32) * spread
    if len(shards) > 0:
        values = block_scale(rng, shape, shards, -0.22, 0.18) * values
    return jnp.clip(values, min=-most, max=most).astype(kind)


def setup_inputs(seed: int = 0) -> dict:
    seeds = jax.random.split(jax.random.key(seed), 13)
    inputs = scatter_about(seeds[0], (TOKENS, D), 1.0, 6.0, ((0, 96),))
    value_cot = scatter_about(seeds[1], (TOKENS, HV), (TOKENS ** -0.5), 0.026977539, ((0, 96), (1, 8)))
    retained = scatter_about(seeds[2], (TOKENS, HV), 1.0, 6.0, ((0, 96), (1, 8)))
    output_cot = scatter_about(seeds[3], (TOKENS, D), (TOKENS ** -0.5), 0.026977539, ((0, 96),))
    proj_value = scatter_about(seeds[4], (D, RANK), D ** -0.5, 0.125, ((0, 96),))
    proj_output = scatter_about(seeds[5], (D, RANK), D ** -0.5, 0.125, ((0, 96),))
    w_value = scatter_about(seeds[6], (D, HV), 1.0, 6.0, ((0, 96), (1, 8)), jnp.float32)
    w_output = scatter_about(seeds[7], (HV, D), 1.0, 6.0, ((0, 8), (1, 96)), jnp.float32)
    first_value = draw_first_value(jax.random.fold_in(seeds[12], 71), 0)
    second_value = jnp.clip(jnp.exp(math.log(4.0) - 2.7725887 * jax.random.uniform(seeds[9], (RANK, HV), jnp.float32) ** block_scale(seeds[9], (RANK, HV), ((0, 96), (1, 8)), -0.2, 0.2)), 0.25, 4.0)
    first_output = draw_first_output(jax.random.fold_in(seeds[12], 71), 0)
    second_output = jnp.clip(jnp.exp(math.log(4.0) - 2.7725887 * jax.random.uniform(seeds[11], (RANK, HV), jnp.float32) ** block_scale(seeds[11], (RANK, HV), ((0, 96), (1, 8)), -0.2, 0.2)), 0.25, 4.0)
    return dict(inputs=inputs, value_cot=value_cot, retained=retained, output_cot=output_cot, proj_value=proj_value, proj_output=proj_output, w_value=w_value, w_output=w_output, first_value=first_value, second_value=second_value, first_output=first_output, second_output=second_output)


beta_one = 0.8
beta_two = 0.9
moment_eps = 1e-08
norm_eps = 1e-06

def adapt(first, second, grad):
    new_first = beta_one * first + (1.0 - beta_one) * grad
    new_second = beta_two * second + (1.0 - beta_two) * grad * grad
    direction = (new_first / (jnp.sqrt(new_second) + moment_eps)).astype(jnp.bfloat16)
    return (new_first, new_second, direction)

def reference(inputs, value_cot, retained, output_cot, proj_value, proj_output, w_value, w_output, first_value, second_value, first_output, second_output):
    x_proj = jnp.dot(inputs, proj_value, preferred_element_type=jnp.float32).astype(jnp.bfloat16)
    o_proj = jnp.dot(output_cot, proj_output, preferred_element_type=jnp.float32).astype(jnp.bfloat16)
    grad_value = jnp.dot(x_proj.T, value_cot, preferred_element_type=jnp.float32)
    grad_output = jnp.dot(o_proj.T, retained, preferred_element_type=jnp.float32)
    first_v, second_v, dir_value = adapt(first_value, second_value, grad_value)
    first_o, second_o, dir_output = adapt(first_output, second_output, grad_output)
    square_v = jnp.sum(jnp.square(dir_value.astype(jnp.float32)))
    square_o = jnp.sum(jnp.square(dir_output.astype(jnp.float32)))
    scale_value = lax.rsqrt(square_v / (RANK * HV) + norm_eps)
    scale_output = lax.rsqrt(square_o / (RANK * HV) + norm_eps)
    step_value = jnp.dot(proj_value, dir_value, preferred_element_type=jnp.float32) * scale_value
    step_output = jnp.dot(dir_output.T, proj_output.T, preferred_element_type=jnp.float32) * scale_output
    copy_value = (w_value + step_value).astype(jnp.bfloat16)
    copy_output = (w_output + step_output).astype(jnp.bfloat16)
    return (step_value, step_output, copy_value, copy_output, first_v, second_v, first_o, second_o)
```

```python
import jax
import jax.numpy as jnp
from jax import lax
from jax.sharding import Mesh
from jax.sharding import PartitionSpec as P

RANK = 192
HV = 4096
FS = ("fs_0", "fs_1")


beta_one = 0.8
beta_two = 0.9
moment_eps = 1e-08
norm_eps = 1e-06


def exchange(pieces, axis):
    return lax.all_to_all(pieces, axis, split_axis=0, concat_axis=0, tiled=True)


def spread(value, axis):
    return exchange(jnp.broadcast_to(value, (lax.axis_size(axis), *value.shape)), axis)


def contract(left, right, dims):
    return lax.dot_general(left, right, (dims, ((), ())), preferred_element_type=jnp.float32)


def adapt(first, second, grad):
    new_first = beta_one * first + (1.0 - beta_one) * grad
    new_second = beta_two * second + (1.0 - beta_two) * grad * grad
    direction = (new_first / (jnp.sqrt(new_second) + moment_eps)).astype(jnp.bfloat16)
    return (new_first, new_second, direction)


def squares(direction):
    return jnp.sum(jnp.square(direction.astype(jnp.float32)))


def per_device(
    inputs,
    value_cot,
    retained,
    output_cot,
    proj_value,
    proj_output,
    w_value,
    w_output,
    first_value,
    second_value,
    first_output,
    second_output,
):
    bf16 = jnp.bfloat16
    rank = proj_value.shape[1]
    columns = value_cot.shape[1]
    early = jnp.concatenate(
        [w_value.astype(bf16), w_output.T.astype(bf16), proj_value, proj_output], axis=1
    )
    early = lax.all_gather(early, FS, axis=0, tiled=True)
    wide_value = early[:, :columns]
    wide_output = early[:, columns : 2 * columns]
    full_value = early[:, 2 * columns : 2 * columns + rank]
    full_output = early[:, 2 * columns + rank :]

    width = rank // lax.axis_size("tp")
    offset = lax.axis_index("tp") * width
    own = jnp.concatenate(
        [
            lax.dynamic_slice_in_dim(proj_value, offset, width, 1),
            lax.dynamic_slice_in_dim(proj_output, offset, width, 1),
        ],
        axis=1,
    )
    rows = spread(own, "fs_0")
    rows = spread(rows.reshape(-1, 2 * width), "fs_1")
    rows = rows.reshape(lax.axis_size("fs_1"), lax.axis_size("fs_0"), -1, 2 * width)
    rows = jnp.swapaxes(rows, 0, 1).reshape(-1, 2 * width)
    narrow = jnp.concatenate(
        [
            contract(rows[:, :width], inputs, ((0,), (1,))),
            contract(rows[:, width:], output_cot, ((0,), (1,))),
        ],
        axis=0,
    ).astype(bf16)
    projected = spread(narrow, "tp")
    x_proj = projected[:, :width].reshape(rank, -1)
    o_proj = projected[:, width:].reshape(rank, -1)

    partial = jnp.concatenate(
        [contract(x_proj, value_cot, ((1,), (0,))), contract(o_proj, retained, ((1,), (0,)))],
        axis=1,
    ).astype(bf16)
    pieces = exchange(partial.reshape(lax.axis_size(FS), -1, 2 * columns), FS)
    summed = pieces.astype(jnp.float32).sum(axis=0)
    first_v, second_v, dir_value = adapt(first_value, second_value, summed[:, :columns])
    first_o, second_o, dir_output = adapt(first_output, second_output, summed[:, columns:])

    dirs = spread(jnp.concatenate([dir_value, dir_output], axis=1), FS).reshape(rank, -1)
    dir_value, dir_output = (dirs[:, :columns], dirs[:, columns:])
    sums = jnp.stack([squares(dir_value), squares(dir_output)])
    totals = spread(sums[None], "tp").sum(axis=(0, 1))
    scale_value = lax.rsqrt(totals[0] / (RANK * HV) + norm_eps)
    scale_output = lax.rsqrt(totals[1] / (RANK * HV) + norm_eps)

    step_value = contract(proj_value, dir_value, ((1,), (0,))) * scale_value
    step_output = contract(dir_output, proj_output, ((0,), (1,))) * scale_output
    copy_value = contract(full_value, dir_value, ((1,), (0,))) * scale_value
    copy_value = (wide_value.astype(jnp.float32) + copy_value).astype(bf16)
    copy_output = contract(dir_output, full_output, ((0,), (1,))) * scale_output
    copy_output = (wide_output.T.astype(jnp.float32) + copy_output).astype(bf16)
    return (step_value, step_output, copy_value, copy_output, first_v, second_v, first_o, second_o)


def solution(mesh):
    split = Mesh(mesh.devices.reshape(12, 8, mesh.shape["tp"]), ("fs_0", "fs_1", "tp"))
    return jax.shard_map(
        per_device,
        mesh=split,
        in_specs=(
            P(FS, None),
            P(FS, "tp"),
            P(FS, "tp"),
            P(FS, None),
            P(FS, None),
            P(FS, None),
            P(FS, "tp"),
            P("tp", FS),
            P(FS, "tp"),
            P(FS, "tp"),
            P(FS, "tp"),
            P(FS, "tp"),
        ),
        out_specs=(
            P(FS, "tp"),
            P("tp", FS),
            P(None, "tp"),
            P("tp", None),
            P(FS, "tp"),
            P(FS, "tp"),
            P(FS, "tp"),
            P(FS, "tp"),
        ),
        check_vma=False,
    )
```

```python
import jax
import jax.numpy as jnp
from jax import lax
from jax.experimental import pallas as pl
from jax.experimental.pallas import tpu as pltpu
from jax.sharding import Mesh
from jax.sharding import PartitionSpec as P

RANK = 192
HV = 4096
FS = ("fs_0", "fs_1")


beta_one = 0.8
beta_two = 0.9
moment_eps = 1e-08
norm_eps = 1e-06


def exchange(pieces, axis):
    return lax.all_to_all(pieces, axis, split_axis=0, concat_axis=0, tiled=True)


def spread(value, axis):
    return exchange(jnp.broadcast_to(value, (lax.axis_size(axis), *value.shape)), axis)


def contract(left, right, dims):
    return lax.dot_general(left, right, (dims, ((), ())), preferred_element_type=jnp.float32)


def adapt(first, second, grad):
    new_first = beta_one * first + (1.0 - beta_one) * grad
    new_second = beta_two * second + (1.0 - beta_two) * grad * grad
    direction = (new_first / (jnp.sqrt(new_second) + moment_eps)).astype(jnp.bfloat16)
    return (new_first, new_second, direction)


def squares(direction):
    return jnp.sum(jnp.square(direction.astype(jnp.float32)))


LANES = 128


def fold_kernel(scale_ref, early_ref, dir_value_ref, dir_output_ref, value_ref, output_ref):
    columns = value_ref.shape[1]
    at = 2 * columns
    left = jnp.concatenate(
        [early_ref[:, at : at + LANES], early_ref[:, at + 2 * LANES : at + 3 * LANES]], axis=1
    )
    update = jnp.dot(left, dir_value_ref[...], preferred_element_type=jnp.float32)
    update = early_ref[:, :columns].astype(jnp.float32) + update * scale_ref[0]
    value_ref[...] = update.astype(value_ref.dtype)
    left = early_ref[:, at + LANES : at + 3 * LANES]
    update = jnp.dot(left, dir_output_ref[...], preferred_element_type=jnp.float32)
    update = early_ref[:, columns:at].astype(jnp.float32) + update * scale_ref[1]
    output_ref[...] = update.astype(output_ref.dtype).T


def fold(scales, early, dir_value, dir_output, tile):
    rows, columns = early.shape[0], dir_value.shape[1]
    gap = jnp.zeros((2 * LANES - dir_value.shape[0], columns), dir_value.dtype)
    wide_value = jnp.concatenate([dir_value, gap], axis=0)
    wide_output = jnp.concatenate([dir_output[:LANES], gap, dir_output[LANES:]], axis=0)
    return pl.pallas_call(
        fold_kernel,
        grid=(rows // tile,),
        in_specs=[
            pl.BlockSpec(memory_space=pltpu.SMEM),
            pl.BlockSpec((tile, early.shape[1]), lambda i: (i, 0)),
            pl.BlockSpec((2 * LANES, columns), lambda i: (0, 0)),
            pl.BlockSpec((2 * LANES, columns), lambda i: (0, 0)),
        ],
        out_specs=[
            pl.BlockSpec((tile, columns), lambda i: (i, 0)),
            pl.BlockSpec((columns, tile), lambda i: (0, i)),
        ],
        out_shape=[
            jax.ShapeDtypeStruct((rows, columns), jnp.bfloat16),
            jax.ShapeDtypeStruct((columns, rows), jnp.bfloat16),
        ],
        name="fold",
    )(scales, early, wide_value, wide_output)


def per_device(
    inputs,
    value_cot,
    retained,
    output_cot,
    proj_value,
    proj_output,
    w_value,
    w_output,
    first_value,
    second_value,
    first_output,
    second_output,
):
    bf16 = jnp.bfloat16
    rank = proj_value.shape[1]
    columns = value_cot.shape[1]
    width = rank // lax.axis_size("tp")
    offset = lax.axis_index("tp") * width

    near = spread(jnp.concatenate([proj_value, proj_output], axis=1), "fs_1")
    near = near.reshape(-1, 2 * rank)
    old = spread(jnp.concatenate([w_value.astype(bf16), w_output.T.astype(bf16)], axis=1), "fs_1")
    old = old.reshape(-1, 2 * columns)
    early = jnp.concatenate(
        [
            old,
            near[:, :LANES],
            near[:, rank : rank + LANES],
            near[:, LANES:rank],
            near[:, rank + LANES :],
        ],
        axis=1,
    )
    early = lax.all_gather(early, "fs_0", axis=0, tiled=True)

    own = jnp.concatenate(
        [
            lax.dynamic_slice_in_dim(near[:, :rank], offset, width, 1),
            lax.dynamic_slice_in_dim(near[:, rank:], offset, width, 1),
        ],
        axis=1,
    )
    rows = spread(own.T, "fs_0")
    rows = jnp.swapaxes(rows, 0, 1).reshape(2 * width, -1)
    narrow = jnp.concatenate(
        [
            contract(rows[:width], inputs, ((1,), (1,))),
            contract(rows[width:], output_cot, ((1,), (1,))),
        ],
        axis=0,
    ).astype(bf16)
    projected = spread(narrow, "tp")
    x_proj = projected[:, :width].reshape(rank, -1)
    o_proj = projected[:, width:].reshape(rank, -1)

    partial = jnp.concatenate(
        [contract(x_proj, value_cot, ((1,), (0,))), contract(o_proj, retained, ((1,), (0,)))],
        axis=1,
    ).astype(bf16)
    pieces = exchange(partial.reshape(lax.axis_size(FS), -1, 2 * columns), FS)
    summed = pieces.astype(jnp.float32).sum(axis=0)
    first_v, second_v, dir_value = adapt(first_value, second_value, summed[:, :columns])
    first_o, second_o, dir_output = adapt(first_output, second_output, summed[:, columns:])

    dirs = spread(jnp.concatenate([dir_value, dir_output], axis=1), FS).reshape(rank, -1)
    dir_value, dir_output = (dirs[:, :columns], dirs[:, columns:])
    sums = jnp.stack([squares(dir_value), squares(dir_output)])
    totals = spread(sums[None], "tp").sum(axis=(0, 1))
    scales = lax.rsqrt(totals / (RANK * HV) + norm_eps)

    step_value = contract(proj_value, dir_value, ((1,), (0,))) * scales[0]
    step_output = contract(dir_output, proj_output, ((0,), (1,))) * scales[1]
    copy_value, copy_output = fold(scales, early, dir_value, dir_output, 768)
    return (step_value, step_output, copy_value, copy_output, first_v, second_v, first_o, second_o)


def solution(mesh):
    split = Mesh(mesh.devices.reshape(12, 8, mesh.shape["tp"]), ("fs_0", "fs_1", "tp"))
    return jax.shard_map(
        per_device,
        mesh=split,
        in_specs=(
            P(FS, None),
            P(FS, "tp"),
            P(FS, "tp"),
            P(FS, None),
            P(FS, None),
            P(FS, None),
            P(FS, "tp"),
            P("tp", FS),
            P(FS, "tp"),
            P(FS, "tp"),
            P(FS, "tp"),
            P(FS, "tp"),
        ),
        out_specs=(
            P(FS, "tp"),
            P("tp", FS),
            P(None, "tp"),
            P("tp", None),
            P(FS, "tp"),
            P(FS, "tp"),
            P(FS, "tp"),
            P(FS, "tp"),
        ),
        check_vma=False,
    )
```

```python
import functools

import jax
import jax.numpy as jnp
from jax import lax
from jax.experimental import pallas as pl
from jax.experimental.pallas import tpu as pltpu
from jax.sharding import Mesh
from jax.sharding import PartitionSpec as P

RANK = 192
HV = 4096
FS = ("fs_0", "fs_1")


beta_one = 0.8
beta_two = 0.9
moment_eps = 1e-08
norm_eps = 1e-06


def exchange(pieces, axis):
    return lax.all_to_all(pieces, axis, split_axis=0, concat_axis=0, tiled=True)


def spread(value, axis):
    return exchange(jnp.broadcast_to(value, (lax.axis_size(axis), *value.shape)), axis)


def contract(left, right, dims):
    return lax.dot_general(left, right, (dims, ((), ())), preferred_element_type=jnp.float32)


def adapt(first, second, grad):
    new_first = beta_one * first + (1.0 - beta_one) * grad
    new_second = beta_two * second + (1.0 - beta_two) * grad * grad
    direction = (new_first / (jnp.sqrt(new_second) + moment_eps)).astype(jnp.bfloat16)
    return (new_first, new_second, direction)


LANES = 128


def fold_kernel(
    count,
    sums_ref,
    early_ref,
    own_value_ref,
    own_output_ref,
    wide_value_ref,
    wide_output_ref,
    dirs_ref,
    value_ref,
    output_ref,
    step_value_ref,
    step_output_ref,
):
    columns = value_ref.shape[1]
    at = 2 * columns

    def scale_of(sums):
        total = jnp.sum(jnp.sum(sums, axis=1, keepdims=True), axis=0, keepdims=True)
        return lax.rsqrt(total / count + norm_eps)

    scale_value = scale_of(sums_ref[:, :columns])
    scale_output = scale_of(sums_ref[:, columns:])

    @pl.when(pl.program_id(0) == 0)
    def _():
        step = jnp.dot(
            own_value_ref[...], dirs_ref[:, :columns], preferred_element_type=jnp.float32
        )
        step_value_ref[...] = step * scale_value
        step = jnp.dot(
            own_output_ref[...], dirs_ref[:, columns:], preferred_element_type=jnp.float32
        )
        step_output_ref[...] = step * scale_output

    left = jnp.concatenate(
        [early_ref[:, at : at + LANES], early_ref[:, at + 2 * LANES : at + 3 * LANES]], axis=1
    )
    update = jnp.dot(left, wide_value_ref[...], preferred_element_type=jnp.float32)
    update = early_ref[:, :columns].astype(jnp.float32) + update * scale_value
    value_ref[...] = update.astype(value_ref.dtype)
    left = early_ref[:, at + LANES : at + 3 * LANES]
    update = jnp.dot(left, wide_output_ref[...], preferred_element_type=jnp.float32)
    update = early_ref[:, columns:at].astype(jnp.float32) + update * scale_output
    output_ref[...] = update.astype(output_ref.dtype).T


def fold(sums, early, proj_value, proj_output, dirs, tile):
    rows, columns = early.shape[0], dirs.shape[1] // 2
    own, rank = proj_value.shape
    gap = jnp.zeros((2 * LANES - rank, columns), dirs.dtype)
    wide_value = jnp.concatenate([dirs[:, :columns], gap], axis=0)
    wide_output = jnp.concatenate([dirs[:LANES, columns:], gap, dirs[LANES:, columns:]], axis=0)

    def whole(*shape):
        return pl.BlockSpec(shape, lambda i: (0, 0))

    out = pl.pallas_call(
        functools.partial(fold_kernel, RANK * HV),
        grid=(rows // tile,),
        in_specs=[
            whole(*sums.shape),
            pl.BlockSpec((tile, early.shape[1]), lambda i: (i, 0)),
            whole(own, rank),
            whole(own, rank),
            whole(2 * LANES, columns),
            whole(2 * LANES, columns),
            whole(rank, 2 * columns),
        ],
        out_specs=[
            pl.BlockSpec((tile, columns), lambda i: (i, 0)),
            pl.BlockSpec((columns, tile), lambda i: (0, i)),
            whole(own, columns),
            whole(own, columns),
        ],
        out_shape=[
            jax.ShapeDtypeStruct((rows, columns), jnp.bfloat16),
            jax.ShapeDtypeStruct((columns, rows), jnp.bfloat16),
            jax.ShapeDtypeStruct((own, columns), jnp.float32),
            jax.ShapeDtypeStruct((own, columns), jnp.float32),
        ],
        name="fold",
    )(sums, early, proj_value, proj_output, wide_value, wide_output, dirs)
    return (out[0], out[1], out[2], out[3].T)


def per_device(
    inputs,
    value_cot,
    retained,
    output_cot,
    proj_value,
    proj_output,
    w_value,
    w_output,
    first_value,
    second_value,
    first_output,
    second_output,
):
    bf16 = jnp.bfloat16
    rank = proj_value.shape[1]
    columns = value_cot.shape[1]
    deep, high = lax.axis_size("fs_0"), lax.axis_size("fs_1")

    piece = [w_value.astype(bf16), w_output.T.astype(bf16)]
    piece += [proj_value[:, :LANES], proj_output[:, :LANES]]
    piece += [proj_value[:, LANES:], proj_output[:, LANES:]]
    near = spread(jnp.concatenate(piece, axis=1), "fs_1")
    near = near.reshape(-1, near.shape[-1])
    early = lax.all_gather(near, "fs_0", axis=0, tiled=True)

    width = rank // lax.axis_size("tp")
    offset = lax.axis_index("tp") * width
    at, rest = 2 * columns, rank - LANES
    last = at + 2 * LANES
    near_value = jnp.concatenate([near[:, at : at + LANES], near[:, last : last + rest]], axis=1)
    near_output = jnp.concatenate([near[:, at + LANES : last], near[:, last + rest :]], axis=1)
    own = jnp.concatenate(
        [
            lax.dynamic_slice_in_dim(near_value, offset, width, 1),
            lax.dynamic_slice_in_dim(near_output, offset, width, 1),
        ],
        axis=1,
    )
    rows = spread(own.T, "fs_0")
    rows = jnp.swapaxes(rows, 0, 1).reshape(2 * width, -1)
    narrow = jnp.concatenate(
        [
            contract(rows[:width], inputs, ((1,), (1,))),
            contract(rows[width:], output_cot, ((1,), (1,))),
        ],
        axis=0,
    ).astype(bf16)
    projected = spread(narrow, "tp")
    x_proj = projected[:, :width].reshape(rank, -1)
    o_proj = projected[:, width:].reshape(rank, -1)

    partial = jnp.concatenate(
        [contract(x_proj, value_cot, ((1,), (0,))), contract(o_proj, retained, ((1,), (0,)))],
        axis=1,
    ).astype(bf16)
    pieces = partial.reshape(deep, high, -1, 2 * columns)
    pieces = exchange(jnp.swapaxes(pieces, 0, 1).reshape(high, -1, 2 * columns), "fs_1")
    pieces = pieces.astype(jnp.float32).sum(axis=0).astype(bf16)
    pieces = exchange(pieces.reshape(deep, -1, 2 * columns), "fs_0")
    summed = pieces.astype(jnp.float32).sum(axis=0)
    first_v, second_v, dir_value = adapt(first_value, second_value, summed[:, :columns])
    first_o, second_o, dir_output = adapt(first_output, second_output, summed[:, columns:])

    dirs = spread(jnp.concatenate([dir_value, dir_output], axis=1), "fs_0")
    dirs = spread(dirs.reshape(-1, 2 * columns), "fs_1")
    sums = jnp.square(dirs.astype(jnp.float32)).sum(axis=(0, 1))
    sums = spread(sums, "tp")
    dirs = dirs.reshape(high, deep, -1, 2 * columns)
    dirs = jnp.swapaxes(dirs, 0, 1).reshape(rank, -1)

    copy_value, copy_output, step_value, step_output = fold(
        sums, early, proj_value, proj_output, dirs, 768
    )
    return (step_value, step_output, copy_value, copy_output, first_v, second_v, first_o, second_o)


def solution(mesh):
    split = Mesh(mesh.devices.reshape(12, 8, mesh.shape["tp"]), ("fs_0", "fs_1", "tp"))
    return jax.shard_map(
        per_device,
        mesh=split,
        in_specs=(
            P(FS, None),
            P(FS, "tp"),
            P(FS, "tp"),
            P(FS, None),
            P(FS, None),
            P(FS, None),
            P(FS, "tp"),
            P("tp", FS),
            P(FS, "tp"),
            P(FS, "tp"),
            P(FS, "tp"),
            P(FS, "tp"),
        ),
        out_specs=(
            P(FS, "tp"),
            P("tp", FS),
            P(None, "tp"),
            P("tp", None),
            P(FS, "tp"),
            P(FS, "tp"),
            P(FS, "tp"),
            P(FS, "tp"),
        ),
        check_vma=False,
    )
```

```python
import functools

import jax
import jax.numpy as jnp
from jax import lax
from jax.experimental import pallas as pl
from jax.experimental.pallas import tpu as pltpu
from jax.sharding import Mesh
from jax.sharding import PartitionSpec as P

RANK = 192
HV = 4096
FS = ("fs_0", "fs_1")


beta_one = 0.8
beta_two = 0.9
moment_eps = 1e-08
norm_eps = 1e-06


def exchange(pieces, axis):
    return lax.all_to_all(pieces, axis, split_axis=0, concat_axis=0, tiled=True)


def spread(value, axis):
    return exchange(jnp.broadcast_to(value, (lax.axis_size(axis), *value.shape)), axis)


def contract(left, right, dims):
    return lax.dot_general(left, right, (dims, ((), ())), preferred_element_type=jnp.float32)


def adapt(first, second, grad):
    new_first = beta_one * first + (1.0 - beta_one) * grad
    new_second = beta_two * second + (1.0 - beta_two) * grad * grad
    direction = (new_first / (jnp.sqrt(new_second) + moment_eps)).astype(jnp.bfloat16)
    return (new_first, new_second, direction)


def fold_kernel(
    count,
    sums_ref,
    early_ref,
    own_value_ref,
    own_output_ref,
    dirs_ref,
    value_ref,
    output_ref,
    step_value_ref,
    step_output_ref,
):
    columns, rank = value_ref.shape[1], own_value_ref.shape[1]
    at = 2 * columns

    def scale_of(sums):
        total = jnp.sum(jnp.sum(sums, axis=1, keepdims=True), axis=0, keepdims=True)
        return lax.rsqrt(total / count + norm_eps)

    scale_value = scale_of(sums_ref[:, :columns])
    scale_output = scale_of(sums_ref[:, columns:])

    @pl.when(pl.program_id(0) == 0)
    def _():
        step = jnp.dot(
            own_value_ref[...], dirs_ref[:, :columns], preferred_element_type=jnp.float32
        )
        step_value_ref[...] = step * scale_value
        step = jnp.dot(
            own_output_ref[...], dirs_ref[:, columns:], preferred_element_type=jnp.float32
        )
        step_output_ref[...] = step * scale_output

    left = early_ref[:, at : at + rank]
    update = jnp.dot(left, dirs_ref[:, :columns], preferred_element_type=jnp.float32)
    update = early_ref[:, :columns].astype(jnp.float32) + update * scale_value
    value_ref[...] = update.astype(value_ref.dtype)
    left = early_ref[:, at + rank :]
    update = jnp.dot(left, dirs_ref[:, columns:], preferred_element_type=jnp.float32)
    update = early_ref[:, columns:at].astype(jnp.float32) + update * scale_output
    output_ref[...] = update.astype(output_ref.dtype).T


def fold(sums, early, proj_value, proj_output, dirs, tile):
    rows, columns = early.shape[0], dirs.shape[1] // 2
    own, rank = proj_value.shape

    def whole(*shape):
        return pl.BlockSpec(shape, lambda i: (0, 0))

    out = pl.pallas_call(
        functools.partial(fold_kernel, RANK * HV),
        grid=(rows // tile,),
        in_specs=[
            whole(*sums.shape),
            pl.BlockSpec((tile, early.shape[1]), lambda i: (i, 0)),
            whole(own, rank),
            whole(own, rank),
            whole(rank, 2 * columns),
        ],
        out_specs=[
            pl.BlockSpec((tile, columns), lambda i: (i, 0)),
            pl.BlockSpec((columns, tile), lambda i: (0, i)),
            whole(own, columns),
            whole(own, columns),
        ],
        out_shape=[
            jax.ShapeDtypeStruct((rows, columns), jnp.bfloat16),
            jax.ShapeDtypeStruct((columns, rows), jnp.bfloat16),
            jax.ShapeDtypeStruct((own, columns), jnp.float32),
            jax.ShapeDtypeStruct((own, columns), jnp.float32),
        ],
        name="fold",
    )(sums, early, proj_value, proj_output, dirs)
    return (out[0], out[1], out[2], out[3].T)


def per_device(
    inputs,
    value_cot,
    retained,
    output_cot,
    proj_value,
    proj_output,
    w_value,
    w_output,
    first_value,
    second_value,
    first_output,
    second_output,
):
    bf16 = jnp.bfloat16
    rank = proj_value.shape[1]
    columns = value_cot.shape[1]
    deep, high = lax.axis_size("fs_0"), lax.axis_size("fs_1")

    piece = [w_value.astype(bf16), w_output.T.astype(bf16), proj_value, proj_output]
    near = spread(jnp.concatenate(piece, axis=1), "fs_1")
    near = near.reshape(-1, near.shape[-1])
    width = rank // lax.axis_size("tp")
    offset = lax.axis_index("tp") * width
    at = 2 * columns
    own = jnp.concatenate(
        [
            lax.dynamic_slice_in_dim(near[:, at : at + rank], offset, width, 1),
            lax.dynamic_slice_in_dim(near[:, at + rank :], offset, width, 1),
        ],
        axis=1,
    )
    rows = spread(own.T, "fs_0")
    near, rows = lax.optimization_barrier((near, rows))
    early = lax.all_gather(near, "fs_0", axis=0, tiled=True)
    rows = jnp.swapaxes(rows, 0, 1).reshape(2 * width, -1)
    narrow = jnp.concatenate(
        [
            contract(rows[:width], inputs, ((1,), (1,))),
            contract(rows[width:], output_cot, ((1,), (1,))),
        ],
        axis=0,
    ).astype(bf16)
    projected = spread(narrow, "tp")
    x_proj = projected[:, :width].reshape(rank, -1)
    o_proj = projected[:, width:].reshape(rank, -1)

    partial = jnp.concatenate(
        [contract(x_proj, value_cot, ((1,), (0,))), contract(o_proj, retained, ((1,), (0,)))],
        axis=1,
    ).astype(bf16)
    pieces = partial.reshape(deep, high, -1, 2 * columns)
    pieces = exchange(jnp.swapaxes(pieces, 0, 1).reshape(high, -1, 2 * columns), "fs_1")
    pieces = pieces.astype(jnp.float32).sum(axis=0).astype(bf16)
    pieces = exchange(pieces.reshape(deep, -1, 2 * columns), "fs_0")
    summed = pieces.astype(jnp.float32).sum(axis=0)
    first_v, second_v, dir_value = adapt(first_value, second_value, summed[:, :columns])
    first_o, second_o, dir_output = adapt(first_output, second_output, summed[:, columns:])

    dirs = spread(jnp.concatenate([dir_value, dir_output], axis=1), "fs_0")
    dirs = spread(dirs.reshape(-1, 2 * columns), "fs_1")
    sums = jnp.square(dirs.astype(jnp.float32)).sum(axis=(0, 1))
    sums = spread(sums, "tp")
    dirs = dirs.reshape(high, deep, -1, 2 * columns)
    dirs = jnp.swapaxes(dirs, 0, 1).reshape(rank, -1)

    copy_value, copy_output, step_value, step_output = fold(
        sums, early, proj_value, proj_output, dirs, 768
    )
    return (step_value, step_output, copy_value, copy_output, first_v, second_v, first_o, second_o)


def solution(mesh):
    split = Mesh(mesh.devices.reshape(12, 8, mesh.shape["tp"]), ("fs_0", "fs_1", "tp"))
    return jax.shard_map(
        per_device,
        mesh=split,
        in_specs=(
            P(FS, None),
            P(FS, "tp"),
            P(FS, "tp"),
            P(FS, None),
            P(FS, None),
            P(FS, None),
            P(FS, "tp"),
            P("tp", FS),
            P(FS, "tp"),
            P(FS, "tp"),
            P(FS, "tp"),
            P(FS, "tp"),
        ),
        out_specs=(
            P(FS, "tp"),
            P("tp", FS),
            P(None, "tp"),
            P("tp", None),
            P(FS, "tp"),
            P(FS, "tp"),
            P(FS, "tp"),
            P(FS, "tp"),
        ),
        check_vma=False,
    )
```

```python
import functools

import jax
import jax.numpy as jnp
from jax import lax
from jax.experimental import pallas as pl
from jax.experimental.pallas import tpu as pltpu
from jax.sharding import Mesh
from jax.sharding import PartitionSpec as P

RANK = 192
HV = 4096
FS = ("fs_0", "fs_1")


beta_one = 0.8
beta_two = 0.9
moment_eps = 1e-08
norm_eps = 1e-06


def exchange(pieces, axis):
    return lax.all_to_all(pieces, axis, split_axis=0, concat_axis=0, tiled=True)


def spread(value, axis):
    return exchange(jnp.broadcast_to(value, (lax.axis_size(axis), *value.shape)), axis)


def contract(left, right, dims):
    return lax.dot_general(left, right, (dims, ((), ())), preferred_element_type=jnp.float32)


def adapt(first, second, grad):
    new_first = beta_one * first + (1.0 - beta_one) * grad
    new_second = beta_two * second + (1.0 - beta_two) * grad * grad
    direction = (new_first / (jnp.sqrt(new_second) + moment_eps)).astype(jnp.bfloat16)
    return (new_first, new_second, direction)


def fold_kernel(
    count,
    sums_ref,
    early_ref,
    own_value_ref,
    own_output_ref,
    dirs_ref,
    value_ref,
    output_ref,
    step_value_ref,
    step_output_ref,
):
    columns, rank = value_ref.shape[1], own_value_ref.shape[1]
    at = 2 * columns

    def scale_of(sums):
        total = jnp.sum(jnp.sum(sums, axis=1, keepdims=True), axis=0, keepdims=True)
        return lax.rsqrt(total / count + norm_eps)

    scale_value = scale_of(sums_ref[:, :columns])
    scale_output = scale_of(sums_ref[:, columns:])

    @pl.when(pl.program_id(0) == 0)
    def _():
        step = jnp.dot(
            own_value_ref[...], dirs_ref[:, :columns], preferred_element_type=jnp.float32
        )
        step_value_ref[...] = step * scale_value
        step = jnp.dot(
            own_output_ref[...], dirs_ref[:, columns:], preferred_element_type=jnp.float32
        )
        step_output_ref[...] = step * scale_output

    left = early_ref[:, at : at + rank]
    update = jnp.dot(left, dirs_ref[:, :columns], preferred_element_type=jnp.float32)
    update = early_ref[:, :columns].astype(jnp.float32) + update * scale_value
    value_ref[...] = update.astype(value_ref.dtype)
    left = early_ref[:, at + rank :]
    update = jnp.dot(left, dirs_ref[:, columns:], preferred_element_type=jnp.float32)
    update = early_ref[:, columns:at].astype(jnp.float32) + update * scale_output
    output_ref[...] = update.astype(output_ref.dtype).T


def fold(sums, early, proj_value, proj_output, dirs, tile):
    rows, columns = early.shape[0], dirs.shape[1] // 2
    own, rank = proj_value.shape

    def whole(*shape):
        return pl.BlockSpec(shape, lambda i: (0, 0))

    out = pl.pallas_call(
        functools.partial(fold_kernel, RANK * HV),
        grid=(rows // tile,),
        in_specs=[
            whole(*sums.shape),
            pl.BlockSpec((tile, early.shape[1]), lambda i: (i, 0)),
            whole(own, rank),
            whole(own, rank),
            whole(rank, 2 * columns),
        ],
        out_specs=[
            pl.BlockSpec((tile, columns), lambda i: (i, 0)),
            pl.BlockSpec((columns, tile), lambda i: (0, i)),
            whole(own, columns),
            whole(own, columns),
        ],
        out_shape=[
            jax.ShapeDtypeStruct((rows, columns), jnp.bfloat16),
            jax.ShapeDtypeStruct((columns, rows), jnp.bfloat16),
            jax.ShapeDtypeStruct((own, columns), jnp.float32),
            jax.ShapeDtypeStruct((own, columns), jnp.float32),
        ],
        name="fold",
    )(sums, early, proj_value, proj_output, dirs)
    return (out[0], out[1], out[2], out[3].T)


def per_device(
    inputs,
    value_cot,
    retained,
    output_cot,
    proj_value,
    proj_output,
    w_value,
    w_output,
    first_value,
    second_value,
    first_output,
    second_output,
):
    bf16 = jnp.bfloat16
    rank = proj_value.shape[1]
    columns = value_cot.shape[1]
    deep, high = lax.axis_size("fs_0"), lax.axis_size("fs_1")

    width = rank // lax.axis_size("tp")
    offset = lax.axis_index("tp") * width
    own = jnp.concatenate(
        [
            lax.dynamic_slice_in_dim(proj_value, offset, width, 1),
            lax.dynamic_slice_in_dim(proj_output, offset, width, 1),
        ],
        axis=1,
    )
    share = spread(own.reshape(-1, proj_value.shape[0] * width), "fs_0")
    share = share.reshape(-1, proj_value.shape[0] * width)
    piece = [w_value.astype(bf16), w_output.T.astype(bf16), proj_value, proj_output, share]
    near = spread(jnp.concatenate(piece, axis=1), "fs_1")
    at = 2 * (columns + rank)
    rows = near[:, :, at:].reshape(high, deep, -1, 2 * width)
    rows = jnp.swapaxes(rows, 0, 1).reshape(-1, 2 * width)
    early = lax.all_gather(near[:, :, :at].reshape(-1, at), "fs_0", axis=0, tiled=True)

    narrow = jnp.concatenate(
        [
            contract(rows[:, :width], inputs, ((0,), (1,))),
            contract(rows[:, width:], output_cot, ((0,), (1,))),
        ],
        axis=0,
    ).astype(bf16)
    projected = spread(narrow, "tp")
    x_proj = projected[:, :width].reshape(rank, -1)
    o_proj = projected[:, width:].reshape(rank, -1)

    partial = jnp.concatenate(
        [contract(x_proj, value_cot, ((1,), (0,))), contract(o_proj, retained, ((1,), (0,)))],
        axis=1,
    ).astype(bf16)
    pieces = partial.reshape(deep, high, -1, 2 * columns)
    pieces = exchange(jnp.swapaxes(pieces, 0, 1).reshape(high, -1, 2 * columns), "fs_1")
    pieces = pieces.astype(jnp.float32).sum(axis=0).astype(bf16)
    pieces = exchange(pieces.reshape(deep, -1, 2 * columns), "fs_0")
    summed = pieces.astype(jnp.float32).sum(axis=0)
    first_v, second_v, dir_value = adapt(first_value, second_value, summed[:, :columns])
    first_o, second_o, dir_output = adapt(first_output, second_output, summed[:, columns:])

    dirs = spread(jnp.concatenate([dir_value, dir_output], axis=1), "fs_0")
    dirs = spread(dirs.reshape(-1, 2 * columns), "fs_1")
    sums = jnp.square(dirs.astype(jnp.float32)).sum(axis=(0, 1))
    sums = spread(sums, "tp")
    dirs = dirs.reshape(high, deep, -1, 2 * columns)
    dirs = jnp.swapaxes(dirs, 0, 1).reshape(rank, -1)

    copy_value, copy_output, step_value, step_output = fold(
        sums, early, proj_value, proj_output, dirs, 768
    )
    return (step_value, step_output, copy_value, copy_output, first_v, second_v, first_o, second_o)


def solution(mesh):
    split = Mesh(mesh.devices.reshape(12, 8, mesh.shape["tp"]), ("fs_0", "fs_1", "tp"))
    return jax.shard_map(
        per_device,
        mesh=split,
        in_specs=(
            P(FS, None),
            P(FS, "tp"),
            P(FS, "tp"),
            P(FS, None),
            P(FS, None),
            P(FS, None),
            P(FS, "tp"),
            P("tp", FS),
            P(FS, "tp"),
            P(FS, "tp"),
            P(FS, "tp"),
            P(FS, "tp"),
        ),
        out_specs=(
            P(FS, "tp"),
            P("tp", FS),
            P(None, "tp"),
            P("tp", None),
            P(FS, "tp"),
            P(FS, "tp"),
            P(FS, "tp"),
            P(FS, "tp"),
        ),
        check_vma=False,
    )
```

```python
import functools

import jax
import jax.numpy as jnp
from jax import lax
from jax.experimental import pallas as pl
from jax.experimental.pallas import tpu as pltpu
from jax.sharding import Mesh
from jax.sharding import PartitionSpec as P

RANK = 192
HV = 4096
FS = ("fs_0", "fs_1")


beta_one = 0.8
beta_two = 0.9
moment_eps = 1e-08
norm_eps = 1e-06


def exchange(pieces, axis):
    return lax.all_to_all(pieces, axis, split_axis=0, concat_axis=0, tiled=True)


def spread(value, axis):
    return exchange(jnp.broadcast_to(value, (lax.axis_size(axis), *value.shape)), axis)


def contract(left, right, dims):
    return lax.dot_general(left, right, (dims, ((), ())), preferred_element_type=jnp.float32)


def adapt(first, second, grad):
    new_first = beta_one * first + (1.0 - beta_one) * grad
    new_second = beta_two * second + (1.0 - beta_two) * grad * grad
    direction = (new_first / (jnp.sqrt(new_second) + moment_eps)).astype(jnp.bfloat16)
    return (new_first, new_second, direction)


def fold_kernel(
    count,
    sums_ref,
    early_ref,
    own_value_ref,
    own_output_ref,
    dirs_ref,
    value_ref,
    output_ref,
    step_value_ref,
    step_output_ref,
):
    columns, rank = value_ref.shape[1], own_value_ref.shape[1]
    at = 2 * columns

    def scale_of(sums):
        total = jnp.sum(jnp.sum(sums, axis=1, keepdims=True), axis=0, keepdims=True)
        return lax.rsqrt(total / count + norm_eps)

    scale_value = scale_of(sums_ref[:, :columns])
    scale_output = scale_of(sums_ref[:, columns:])

    @pl.when(pl.program_id(0) == 0)
    def _():
        step = jnp.dot(
            own_value_ref[...], dirs_ref[:, :columns], preferred_element_type=jnp.float32
        )
        step_value_ref[...] = step * scale_value
        step = jnp.dot(
            own_output_ref[...], dirs_ref[:, columns:], preferred_element_type=jnp.float32
        )
        step_output_ref[...] = step * scale_output

    left = early_ref[:, at : at + rank]
    update = jnp.dot(left, dirs_ref[:, :columns], preferred_element_type=jnp.float32)
    update = early_ref[:, :columns].astype(jnp.float32) + update * scale_value
    value_ref[...] = update.astype(value_ref.dtype)
    left = early_ref[:, at + rank :]
    update = jnp.dot(left, dirs_ref[:, columns:], preferred_element_type=jnp.float32)
    update = early_ref[:, columns:at].astype(jnp.float32) + update * scale_output
    output_ref[...] = update.astype(output_ref.dtype).T


def fold(sums, early, proj_value, proj_output, dirs, tile):
    rows, columns = early.shape[0], dirs.shape[1] // 2
    own, rank = proj_value.shape

    def whole(*shape):
        return pl.BlockSpec(shape, lambda i: (0, 0))

    out = pl.pallas_call(
        functools.partial(fold_kernel, RANK * HV),
        grid=(rows // tile,),
        in_specs=[
            whole(*sums.shape),
            pl.BlockSpec((tile, early.shape[1]), lambda i: (i, 0)),
            whole(own, rank),
            whole(own, rank),
            whole(rank, 2 * columns),
        ],
        out_specs=[
            pl.BlockSpec((tile, columns), lambda i: (i, 0)),
            pl.BlockSpec((columns, tile), lambda i: (0, i)),
            whole(own, columns),
            whole(own, columns),
        ],
        out_shape=[
            jax.ShapeDtypeStruct((rows, columns), jnp.bfloat16),
            jax.ShapeDtypeStruct((columns, rows), jnp.bfloat16),
            jax.ShapeDtypeStruct((own, columns), jnp.float32),
            jax.ShapeDtypeStruct((own, columns), jnp.float32),
        ],
        name="fold",
    )(sums, early, proj_value, proj_output, dirs)
    return (out[0], out[1], out[2], out[3].T)


def per_device(
    inputs,
    value_cot,
    retained,
    output_cot,
    proj_value,
    proj_output,
    w_value,
    w_output,
    first_value,
    second_value,
    first_output,
    second_output,
):
    bf16 = jnp.bfloat16
    rank = proj_value.shape[1]
    columns = value_cot.shape[1]
    deep, high = lax.axis_size("fs_0"), lax.axis_size("fs_1")

    width = rank // lax.axis_size("tp")
    offset = lax.axis_index("tp") * width
    own = jnp.concatenate(
        [
            lax.dynamic_slice_in_dim(proj_value, offset, width, 1),
            lax.dynamic_slice_in_dim(proj_output, offset, width, 1),
        ],
        axis=1,
    )
    share = spread(own.reshape(-1, proj_value.shape[0] * width), "fs_0")
    share = share.reshape(-1, proj_value.shape[0] * width)
    piece = [w_value.astype(bf16), w_output.T.astype(bf16), proj_value, proj_output, share]
    near = lax.all_gather(jnp.concatenate(piece, axis=1), "fs_1")
    at = 2 * (columns + rank)
    rows = near[:, :, at:].reshape(high, deep, -1, 2 * width)
    rows = jnp.swapaxes(rows, 0, 1).reshape(-1, 2 * width)
    early = lax.all_gather(near[:, :, :at].reshape(-1, at), "fs_0", axis=0, tiled=True)

    narrow = jnp.concatenate(
        [
            contract(rows[:, :width], inputs, ((0,), (1,))),
            contract(rows[:, width:], output_cot, ((0,), (1,))),
        ],
        axis=0,
    ).astype(bf16)
    projected = spread(narrow, "tp")
    x_proj = projected[:, :width].reshape(rank, -1)
    o_proj = projected[:, width:].reshape(rank, -1)

    partial = jnp.concatenate(
        [contract(x_proj, value_cot, ((1,), (0,))), contract(o_proj, retained, ((1,), (0,)))],
        axis=1,
    ).astype(bf16)
    pieces = partial.reshape(deep, high, -1, 2 * columns)
    pieces = exchange(jnp.swapaxes(pieces, 0, 1).reshape(high, -1, 2 * columns), "fs_1")
    pieces = pieces.astype(jnp.float32).sum(axis=0).astype(bf16)
    pieces = exchange(pieces.reshape(deep, -1, 2 * columns), "fs_0")
    summed = pieces.astype(jnp.float32).sum(axis=0)
    first_v, second_v, dir_value = adapt(first_value, second_value, summed[:, :columns])
    first_o, second_o, dir_output = adapt(first_output, second_output, summed[:, columns:])

    dirs = spread(jnp.concatenate([dir_value, dir_output], axis=1), "fs_0")
    dirs = lax.all_gather(dirs.reshape(-1, 2 * columns), "fs_1")
    sums = jnp.square(dirs.astype(jnp.float32)).sum(axis=(0, 1))
    sums = spread(sums, "tp")
    dirs = dirs.reshape(high, deep, -1, 2 * columns)
    dirs = jnp.swapaxes(dirs, 0, 1).reshape(rank, -1)

    copy_value, copy_output, step_value, step_output = fold(
        sums, early, proj_value, proj_output, dirs, 768
    )
    return (step_value, step_output, copy_value, copy_output, first_v, second_v, first_o, second_o)


def solution(mesh):
    split = Mesh(mesh.devices.reshape(12, 8, mesh.shape["tp"]), ("fs_0", "fs_1", "tp"))
    return jax.shard_map(
        per_device,
        mesh=split,
        in_specs=(
            P(FS, None),
            P(FS, "tp"),
            P(FS, "tp"),
            P(FS, None),
            P(FS, None),
            P(FS, None),
            P(FS, "tp"),
            P("tp", FS),
            P(FS, "tp"),
            P(FS, "tp"),
            P(FS, "tp"),
            P(FS, "tp"),
        ),
        out_specs=(
            P(FS, "tp"),
            P("tp", FS),
            P(None, "tp"),
            P("tp", None),
            P(FS, "tp"),
            P(FS, "tp"),
            P(FS, "tp"),
            P(FS, "tp"),
        ),
        check_vma=False,
    )
```

```python
import functools

import jax
import jax.numpy as jnp
from jax import lax
from jax.experimental import pallas as pl
from jax.experimental.pallas import tpu as pltpu
from jax.sharding import Mesh
from jax.sharding import PartitionSpec as P

RANK = 192
HV = 4096
FS = ("fs_0", "fs_1")


beta_one = 0.8
beta_two = 0.9
moment_eps = 1e-08
norm_eps = 1e-06


def exchange(pieces, axis):
    return lax.all_to_all(pieces, axis, split_axis=0, concat_axis=0, tiled=True)


def spread(value, axis):
    return exchange(jnp.broadcast_to(value, (lax.axis_size(axis), *value.shape)), axis)


def contract(left, right, dims):
    return lax.dot_general(left, right, (dims, ((), ())), preferred_element_type=jnp.float32)


def adapt(first, second, grad):
    new_first = beta_one * first + (1.0 - beta_one) * grad
    new_second = beta_two * second + (1.0 - beta_two) * grad * grad
    direction = (new_first / (jnp.sqrt(new_second) + moment_eps)).astype(jnp.bfloat16)
    return (new_first, new_second, direction)


def fold_kernel(
    count,
    sums_ref,
    early_ref,
    own_value_ref,
    own_output_ref,
    dirs_ref,
    value_ref,
    output_ref,
    step_value_ref,
    step_output_ref,
):
    columns, rank = value_ref.shape[1], own_value_ref.shape[1]
    at = 2 * columns

    def scale_of(sums):
        total = jnp.sum(jnp.sum(sums, axis=1, keepdims=True), axis=0, keepdims=True)
        return lax.rsqrt(total / count + norm_eps)

    scale_value = scale_of(sums_ref[:, :columns])
    scale_output = scale_of(sums_ref[:, columns:])

    @pl.when(pl.program_id(0) == 0)
    def _():
        step = jnp.dot(
            own_value_ref[...], dirs_ref[:, :columns], preferred_element_type=jnp.float32
        )
        step_value_ref[...] = step * scale_value
        step = jnp.dot(
            own_output_ref[...], dirs_ref[:, columns:], preferred_element_type=jnp.float32
        )
        step_output_ref[...] = step * scale_output

    left = early_ref[:, at : at + rank]
    update = jnp.dot(left, dirs_ref[:, :columns], preferred_element_type=jnp.float32)
    update = early_ref[:, :columns].astype(jnp.float32) + update * scale_value
    value_ref[...] = update.astype(value_ref.dtype)
    left = early_ref[:, at + rank :]
    update = jnp.dot(left, dirs_ref[:, columns:], preferred_element_type=jnp.float32)
    update = early_ref[:, columns:at].astype(jnp.float32) + update * scale_output
    output_ref[...] = update.astype(output_ref.dtype).T


def fold(sums, early, proj_value, proj_output, dirs, tile):
    rows, columns = early.shape[0], dirs.shape[1] // 2
    own, rank = proj_value.shape

    def whole(*shape):
        return pl.BlockSpec(shape, lambda i: (0, 0))

    out = pl.pallas_call(
        functools.partial(fold_kernel, RANK * HV),
        grid=(rows // tile,),
        in_specs=[
            whole(*sums.shape),
            pl.BlockSpec((tile, early.shape[1]), lambda i: (i, 0)),
            whole(own, rank),
            whole(own, rank),
            whole(rank, 2 * columns),
        ],
        out_specs=[
            pl.BlockSpec((tile, columns), lambda i: (i, 0)),
            pl.BlockSpec((columns, tile), lambda i: (0, i)),
            whole(own, columns),
            whole(own, columns),
        ],
        out_shape=[
            jax.ShapeDtypeStruct((rows, columns), jnp.bfloat16),
            jax.ShapeDtypeStruct((columns, rows), jnp.bfloat16),
            jax.ShapeDtypeStruct((own, columns), jnp.float32),
            jax.ShapeDtypeStruct((own, columns), jnp.float32),
        ],
        name="fold",
    )(sums, early, proj_value, proj_output, dirs)
    return (out[0], out[1], out[2], out[3].T)


def per_device(
    inputs,
    value_cot,
    retained,
    output_cot,
    proj_value,
    proj_output,
    w_value,
    w_output,
    first_value,
    second_value,
    first_output,
    second_output,
):
    bf16 = jnp.bfloat16
    rank = proj_value.shape[1]
    columns = value_cot.shape[1]
    deep, high = lax.axis_size("fs_0"), lax.axis_size("fs_1")

    width = rank // lax.axis_size("tp")
    offset = lax.axis_index("tp") * width
    own = jnp.concatenate(
        [
            lax.dynamic_slice_in_dim(proj_value, offset, width, 1),
            lax.dynamic_slice_in_dim(proj_output, offset, width, 1),
        ],
        axis=1,
    )
    rows = spread(own.reshape(-1, proj_value.shape[0] * width), FS).reshape(-1, 2 * width)
    piece = [w_value.astype(bf16), w_output.T.astype(bf16), proj_value, proj_output]
    piece, rows = lax.optimization_barrier((jnp.concatenate(piece, axis=1), rows))
    near = spread(piece, "fs_1")
    narrow = jnp.concatenate(
        [
            contract(rows[:, :width], inputs, ((0,), (1,))),
            contract(rows[:, width:], output_cot, ((0,), (1,))),
        ],
        axis=0,
    ).astype(bf16)
    near, narrow = lax.optimization_barrier((near, narrow))
    early = lax.all_gather(near.reshape(-1, near.shape[-1]), "fs_0", axis=0, tiled=True)

    projected = spread(narrow, "tp")
    x_proj = projected[:, :width].reshape(rank, -1)
    o_proj = projected[:, width:].reshape(rank, -1)

    partial = jnp.concatenate(
        [contract(x_proj, value_cot, ((1,), (0,))), contract(o_proj, retained, ((1,), (0,)))],
        axis=1,
    ).astype(bf16)
    pieces = partial.reshape(deep, high, -1, 2 * columns)
    pieces = exchange(jnp.swapaxes(pieces, 0, 1).reshape(high, -1, 2 * columns), "fs_1")
    pieces = pieces.astype(jnp.float32).sum(axis=0).astype(bf16)
    pieces = exchange(pieces.reshape(deep, -1, 2 * columns), "fs_0")
    summed = pieces.astype(jnp.float32).sum(axis=0)
    first_v, second_v, dir_value = adapt(first_value, second_value, summed[:, :columns])
    first_o, second_o, dir_output = adapt(first_output, second_output, summed[:, columns:])

    dirs = spread(jnp.concatenate([dir_value, dir_output], axis=1), "fs_0")
    dirs = spread(dirs.reshape(-1, 2 * columns), "fs_1")
    sums = jnp.square(dirs.astype(jnp.float32)).sum(axis=(0, 1))
    sums = spread(sums, "tp")
    dirs = dirs.reshape(high, deep, -1, 2 * columns)
    dirs = jnp.swapaxes(dirs, 0, 1).reshape(rank, -1)

    copy_value, copy_output, step_value, step_output = fold(
        sums, early, proj_value, proj_output, dirs, 768
    )
    return (step_value, step_output, copy_value, copy_output, first_v, second_v, first_o, second_o)


def solution(mesh):
    split = Mesh(mesh.devices.reshape(12, 8, mesh.shape["tp"]), ("fs_0", "fs_1", "tp"))
    return jax.shard_map(
        per_device,
        mesh=split,
        in_specs=(
            P(FS, None),
            P(FS, "tp"),
            P(FS, "tp"),
            P(FS, None),
            P(FS, None),
            P(FS, None),
            P(FS, "tp"),
            P("tp", FS),
            P(FS, "tp"),
            P(FS, "tp"),
            P(FS, "tp"),
            P(FS, "tp"),
        ),
        out_specs=(
            P(FS, "tp"),
            P("tp", FS),
            P(None, "tp"),
            P("tp", None),
            P(FS, "tp"),
            P(FS, "tp"),
            P(FS, "tp"),
            P(FS, "tp"),
        ),
        check_vma=False,
    )
```

```python
import functools

import jax
import jax.numpy as jnp
from jax import lax
from jax.experimental import pallas as pl
from jax.experimental.pallas import tpu as pltpu
from jax.sharding import Mesh
from jax.sharding import PartitionSpec as P

RANK = 192
HV = 4096
FS = ("fs_0", "fs_1")


beta_one = 0.8
beta_two = 0.9
moment_eps = 1e-08
norm_eps = 1e-06


def exchange(pieces, axis):
    return lax.all_to_all(pieces, axis, split_axis=0, concat_axis=0, tiled=True)


def spread(value, axis):
    return exchange(jnp.broadcast_to(value, (lax.axis_size(axis), *value.shape)), axis)


def contract(left, right, dims):
    return lax.dot_general(left, right, (dims, ((), ())), preferred_element_type=jnp.float32)


def adapt(first, second, grad):
    new_first = beta_one * first + (1.0 - beta_one) * grad
    new_second = beta_two * second + (1.0 - beta_two) * grad * grad
    direction = (new_first / (jnp.sqrt(new_second) + moment_eps)).astype(jnp.bfloat16)
    return (new_first, new_second, direction)


def fold_kernel(
    count,
    sums_ref,
    early_ref,
    own_value_ref,
    own_output_ref,
    dirs_ref,
    value_ref,
    output_ref,
    step_value_ref,
    step_output_ref,
):
    columns, rank = value_ref.shape[1], own_value_ref.shape[1]
    at = 2 * columns

    def scale_of(sums):
        total = jnp.sum(sums, axis=0)
        total = jnp.sum(jnp.sum(total, axis=1, keepdims=True), axis=0, keepdims=True)
        return lax.rsqrt(total / count + norm_eps)

    half = sums_ref.shape[1] // 2
    scale_value = scale_of(sums_ref[:, :half])
    scale_output = scale_of(sums_ref[:, half:])

    @pl.when(pl.program_id(0) == 0)
    def _():
        step = jnp.dot(
            own_value_ref[...], dirs_ref[:, :columns], preferred_element_type=jnp.float32
        )
        step_value_ref[...] = step * scale_value
        step = jnp.dot(
            own_output_ref[...], dirs_ref[:, columns:], preferred_element_type=jnp.float32
        )
        step_output_ref[...] = step * scale_output

    left = early_ref[:, at : at + rank]
    update = jnp.dot(left, dirs_ref[:, :columns], preferred_element_type=jnp.float32)
    update = early_ref[:, :columns].astype(jnp.float32) + update * scale_value
    value_ref[...] = update.astype(value_ref.dtype)
    left = early_ref[:, at + rank :]
    update = jnp.dot(left, dirs_ref[:, columns:], preferred_element_type=jnp.float32)
    update = early_ref[:, columns:at].astype(jnp.float32) + update * scale_output
    output_ref[...] = update.astype(output_ref.dtype).T


def fold(sums, early, proj_value, proj_output, dirs, tile):
    rows, columns = early.shape[0], dirs.shape[1] // 2
    own, rank = proj_value.shape

    def whole(*shape):
        return pl.BlockSpec(shape, lambda i: (0, 0))

    out = pl.pallas_call(
        functools.partial(fold_kernel, RANK * HV),
        grid=(rows // tile,),
        in_specs=[
            pl.BlockSpec(sums.shape, lambda i: (0, 0, 0)),
            pl.BlockSpec((tile, early.shape[1]), lambda i: (i, 0)),
            whole(own, rank),
            whole(own, rank),
            whole(rank, 2 * columns),
        ],
        out_specs=[
            pl.BlockSpec((tile, columns), lambda i: (i, 0)),
            pl.BlockSpec((columns, tile), lambda i: (0, i)),
            whole(own, columns),
            whole(own, columns),
        ],
        out_shape=[
            jax.ShapeDtypeStruct((rows, columns), jnp.bfloat16),
            jax.ShapeDtypeStruct((columns, rows), jnp.bfloat16),
            jax.ShapeDtypeStruct((own, columns), jnp.float32),
            jax.ShapeDtypeStruct((own, columns), jnp.float32),
        ],
        name="fold",
    )(sums, early, proj_value, proj_output, dirs)
    return (out[0], out[1], out[2], out[3].T)


def per_device(
    inputs,
    value_cot,
    retained,
    output_cot,
    proj_value,
    proj_output,
    w_value,
    w_output,
    first_value,
    second_value,
    first_output,
    second_output,
):
    bf16 = jnp.bfloat16
    rank = proj_value.shape[1]
    columns = value_cot.shape[1]
    deep, high = lax.axis_size("fs_0"), lax.axis_size("fs_1")

    piece = [w_value.astype(bf16), w_output.T.astype(bf16), proj_value, proj_output]
    early = lax.all_gather(jnp.concatenate(piece, axis=1), FS, axis=0, tiled=True)

    width = rank // lax.axis_size("tp")
    offset = lax.axis_index("tp") * width
    own = jnp.concatenate(
        [
            lax.dynamic_slice_in_dim(proj_value, offset, width, 1),
            lax.dynamic_slice_in_dim(proj_output, offset, width, 1),
        ],
        axis=1,
    )
    share = spread(own.reshape(-1, proj_value.shape[0] * width), "fs_0")
    share = spread(share.reshape(-1, proj_value.shape[0] * width), "fs_1")
    rows = share.reshape(high, deep, -1, 2 * width)
    rows = jnp.swapaxes(rows, 0, 1).reshape(-1, 2 * width)

    narrow = jnp.concatenate(
        [
            contract(rows[:, :width], inputs, ((0,), (1,))),
            contract(rows[:, width:], output_cot, ((0,), (1,))),
        ],
        axis=0,
    ).astype(bf16)
    projected = spread(narrow, "tp")
    x_proj = projected[:, :width].reshape(rank, -1)
    o_proj = projected[:, width:].reshape(rank, -1)

    partial = jnp.concatenate(
        [contract(x_proj, value_cot, ((1,), (0,))), contract(o_proj, retained, ((1,), (0,)))],
        axis=1,
    ).astype(bf16)
    pieces = partial.reshape(deep, high, -1, 2 * columns)
    pieces = exchange(jnp.swapaxes(pieces, 0, 1).reshape(high, -1, 2 * columns), "fs_1")
    pieces = pieces.astype(jnp.float32).sum(axis=0).astype(bf16)
    pieces = exchange(pieces.reshape(deep, -1, 2 * columns), "fs_0")
    summed = pieces.astype(jnp.float32).sum(axis=0)
    first_v, second_v, dir_value = adapt(first_value, second_value, summed[:, :columns])
    first_o, second_o, dir_output = adapt(first_output, second_output, summed[:, columns:])

    dirs = spread(jnp.concatenate([dir_value, dir_output], axis=1), "fs_0")
    dirs = spread(dirs.reshape(-1, 2 * columns), "fs_1")
    sums = jnp.square(dirs.astype(jnp.float32)).sum(axis=(0, 1))
    sums = spread(sums.reshape(-1, 128), "tp")
    dirs = dirs.reshape(high, deep, -1, 2 * columns)
    dirs = jnp.swapaxes(dirs, 0, 1).reshape(rank, -1)

    copy_value, copy_output, step_value, step_output = fold(
        sums, early, proj_value, proj_output, dirs, 768
    )
    return (step_value, step_output, copy_value, copy_output, first_v, second_v, first_o, second_o)


def solution(mesh):
    split = Mesh(mesh.devices.reshape(12, 8, mesh.shape["tp"]), ("fs_0", "fs_1", "tp"))
    return jax.shard_map(
        per_device,
        mesh=split,
        in_specs=(
            P(FS, None),
            P(FS, "tp"),
            P(FS, "tp"),
            P(FS, None),
            P(FS, None),
            P(FS, None),
            P(FS, "tp"),
            P("tp", FS),
            P(FS, "tp"),
            P(FS, "tp"),
            P(FS, "tp"),
            P(FS, "tp"),
        ),
        out_specs=(
            P(FS, "tp"),
            P("tp", FS),
            P(None, "tp"),
            P("tp", None),
            P(FS, "tp"),
            P(FS, "tp"),
            P(FS, "tp"),
            P(FS, "tp"),
        ),
        check_vma=False,
    )
```

```python
import functools

import jax
import jax.numpy as jnp
from jax import lax
from jax.experimental import pallas as pl
from jax.experimental.pallas import tpu as pltpu
from jax.sharding import Mesh
from jax.sharding import PartitionSpec as P

RANK = 192
HV = 4096
FS = ("fs_0", "fs_1")


beta_one = 0.8
beta_two = 0.9
moment_eps = 1e-08
norm_eps = 1e-06


def exchange(pieces, axis):
    return lax.all_to_all(pieces, axis, split_axis=0, concat_axis=0, tiled=True)


def spread(value, axis):
    return exchange(jnp.broadcast_to(value, (lax.axis_size(axis), *value.shape)), axis)


def contract(left, right, dims):
    return lax.dot_general(left, right, (dims, ((), ())), preferred_element_type=jnp.float32)


def adapt(first, second, grad):
    new_first = beta_one * first + (1.0 - beta_one) * grad
    new_second = beta_two * second + (1.0 - beta_two) * grad * grad
    direction = (new_first / (jnp.sqrt(new_second) + moment_eps)).astype(jnp.bfloat16)
    return (new_first, new_second, direction)


def fold_kernel(
    count,
    sums_ref,
    early_ref,
    own_value_ref,
    own_output_ref,
    dirs_ref,
    value_ref,
    output_ref,
    step_value_ref,
    step_output_ref,
):
    columns, rank = value_ref.shape[1], own_value_ref.shape[1]
    at = 2 * columns

    def scale_of(sums):
        total = jnp.sum(sums, axis=0)
        total = jnp.sum(jnp.sum(total, axis=1, keepdims=True), axis=0, keepdims=True)
        return lax.rsqrt(total / count + norm_eps)

    half = sums_ref.shape[1] // 2
    scale_value = scale_of(sums_ref[:, :half])
    scale_output = scale_of(sums_ref[:, half:])

    @pl.when(pl.program_id(0) == 0)
    def _():
        step = jnp.dot(
            own_value_ref[...], dirs_ref[:, :columns], preferred_element_type=jnp.float32
        )
        step_value_ref[...] = step * scale_value
        step = jnp.dot(
            own_output_ref[...], dirs_ref[:, columns:], preferred_element_type=jnp.float32
        )
        step_output_ref[...] = step * scale_output

    left = early_ref[:, at : at + rank]
    update = jnp.dot(left, dirs_ref[:, :columns], preferred_element_type=jnp.float32)
    update = early_ref[:, :columns].astype(jnp.float32) + update * scale_value
    value_ref[...] = update.astype(value_ref.dtype)
    left = early_ref[:, at + rank :]
    update = jnp.dot(left, dirs_ref[:, columns:], preferred_element_type=jnp.float32)
    update = early_ref[:, columns:at].astype(jnp.float32) + update * scale_output
    output_ref[...] = update.astype(output_ref.dtype).T


def fold(sums, early, proj_value, proj_output, dirs, tile):
    rows, columns = early.shape[0], dirs.shape[1] // 2
    own, rank = proj_value.shape

    def whole(*shape):
        return pl.BlockSpec(shape, lambda i: (0, 0))

    out = pl.pallas_call(
        functools.partial(fold_kernel, RANK * HV),
        grid=(rows // tile,),
        in_specs=[
            pl.BlockSpec(sums.shape, lambda i: (0, 0, 0)),
            pl.BlockSpec((tile, early.shape[1]), lambda i: (i, 0)),
            whole(own, rank),
            whole(own, rank),
            whole(rank, 2 * columns),
        ],
        out_specs=[
            pl.BlockSpec((tile, columns), lambda i: (i, 0)),
            pl.BlockSpec((columns, tile), lambda i: (0, i)),
            whole(own, columns),
            whole(own, columns),
        ],
        out_shape=[
            jax.ShapeDtypeStruct((rows, columns), jnp.bfloat16),
            jax.ShapeDtypeStruct((columns, rows), jnp.bfloat16),
            jax.ShapeDtypeStruct((own, columns), jnp.float32),
            jax.ShapeDtypeStruct((own, columns), jnp.float32),
        ],
        name="fold",
    )(sums, early, proj_value, proj_output, dirs)
    return (out[0], out[1], out[2], out[3].T)


def per_device(
    inputs,
    value_cot,
    retained,
    output_cot,
    proj_value,
    proj_output,
    w_value,
    w_output,
    first_value,
    second_value,
    first_output,
    second_output,
):
    bf16 = jnp.bfloat16
    rank = proj_value.shape[1]
    columns = value_cot.shape[1]
    deep, high = lax.axis_size("fs_0"), lax.axis_size("fs_1")

    width = rank // lax.axis_size("tp")
    offset = lax.axis_index("tp") * width
    own = jnp.concatenate(
        [
            lax.dynamic_slice_in_dim(proj_value, offset, width, 1),
            lax.dynamic_slice_in_dim(proj_output, offset, width, 1),
        ],
        axis=1,
    )
    share = spread(own.reshape(-1, proj_value.shape[0] * width), "fs_0")
    share = share.reshape(-1, proj_value.shape[0] * width)
    piece = [w_value.astype(bf16), w_output.T.astype(bf16), proj_value, proj_output, share]
    near = spread(jnp.concatenate(piece, axis=1), "fs_1")
    at = 2 * (columns + rank)
    rows = near[:, :, at:].reshape(high, deep, -1, 2 * width)
    rows = jnp.swapaxes(rows, 0, 1).reshape(-1, 2 * width)
    early = lax.all_gather(near[:, :, :at].reshape(-1, at), "fs_0", axis=0, tiled=True)

    narrow = jnp.concatenate(
        [
            contract(rows[:, :width], inputs, ((0,), (1,))),
            contract(rows[:, width:], output_cot, ((0,), (1,))),
        ],
        axis=0,
    ).astype(bf16)
    projected = spread(narrow, "tp")
    x_proj = projected[:, :width].reshape(rank, -1)
    o_proj = projected[:, width:].reshape(rank, -1)

    partial = jnp.concatenate(
        [contract(x_proj, value_cot, ((1,), (0,))), contract(o_proj, retained, ((1,), (0,)))],
        axis=1,
    ).astype(bf16)
    pieces = partial.reshape(deep, high, -1, 2 * columns)
    pieces = exchange(jnp.swapaxes(pieces, 0, 1).reshape(high, -1, 2 * columns), "fs_1")
    pieces = pieces.astype(jnp.float32).sum(axis=0).astype(bf16)
    pieces = exchange(pieces.reshape(deep, -1, 2 * columns), "fs_0")
    summed = pieces.astype(jnp.float32).sum(axis=0)
    first_v, second_v, dir_value = adapt(first_value, second_value, summed[:, :columns])
    first_o, second_o, dir_output = adapt(first_output, second_output, summed[:, columns:])

    dirs = spread(jnp.concatenate([dir_value, dir_output], axis=1), "fs_0")
    dirs = spread(dirs.reshape(-1, 2 * columns), "fs_1")
    sums = jnp.square(dirs.astype(jnp.float32)).sum(axis=(0, 1))
    sums = spread(sums.reshape(-1, 128), "tp")
    dirs = dirs.reshape(high, deep, -1, 2 * columns)
    dirs = jnp.swapaxes(dirs, 0, 1).reshape(rank, -1)

    copy_value, copy_output, step_value, step_output = fold(
        sums, early, proj_value, proj_output, dirs, 768
    )
    return (step_value, step_output, copy_value, copy_output, first_v, second_v, first_o, second_o)


def solution(mesh):
    split = Mesh(mesh.devices.reshape(12, 8, mesh.shape["tp"]), ("fs_0", "fs_1", "tp"))
    return jax.shard_map(
        per_device,
        mesh=split,
        in_specs=(
            P(FS, None),
            P(FS, "tp"),
            P(FS, "tp"),
            P(FS, None),
            P(FS, None),
            P(FS, None),
            P(FS, "tp"),
            P("tp", FS),
            P(FS, "tp"),
            P(FS, "tp"),
            P(FS, "tp"),
            P(FS, "tp"),
        ),
        out_specs=(
            P(FS, "tp"),
            P("tp", FS),
            P(None, "tp"),
            P("tp", None),
            P(FS, "tp"),
            P(FS, "tp"),
            P(FS, "tp"),
            P(FS, "tp"),
        ),
        check_vma=False,
    )
```
